32 devices in a mesh: grp: 2 (over y), fs: 4 (over z), tp: 4 (over x, core).
Axes of the slice: x: 2, y: 2, z: 4, core: 2. Of those that a mesh axis runs over, the one named last changes fastest.
Arguments:
- prompt: bfloat16 [8, 1024, 2048], P(('grp', 'tp')), parts along dimension 0, may hold values from -6 to 6
- gate_first: float32 [2048, 5632], P('fs', 'tp'), may hold values from -0.125 to 0.125
- up_first: float32 [2048, 5632], P('fs', 'tp'), may hold values from -0.125 to 0.125
- down_first: float32 [5632, 2048], P('fs', 'tp'), may hold values from -0.3125 to 0.3125
- norm_gain: float32 [2048], replicated, may hold values from 0.1 to 1.9
- gate_second: float32 [2048, 5632], P('fs', 'tp'), may hold values from -0.125 to 0.125
- up_second: float32 [2048, 5632], P('fs', 'tp'), may hold values from -0.125 to 0.125
- down_second: float32 [5632, 2048], P('fs', 'tp'), may hold values from -0.3125 to 0.3125
Outputs:
- result: bfloat16 [8, 1024, 2048], P(('grp', 'tp'), 'fs'), parts along dimension 0
- gate_one: bfloat16 [4096, 5632], P('grp', 'fs'), parts along dimension 0
- up_one: bfloat16 [4096, 5632], P('grp', 'fs'), parts along dimension 0
- down_one: bfloat16 [5632, 4096], P('fs', 'grp'), parts along dimension 1
- gate_two: bfloat16 [4096, 5632], P('grp', 'fs'), parts along dimension 0
- up_two: bfloat16 [4096, 5632], P('grp', 'fs'), parts along dimension 0
- down_two: bfloat16 [5632, 4096], P('fs', 'grp'), parts along dimension 1
The draws below stay inside these ranges and needn't reach their ends.
There are 2 independent parts, one for each index of `grp`. The reference program is written for one: setup_inputs(seed, part) draws one part's arguments, and reference() takes and returns one part's arrays. A program takes and returns all parts, laid end to end along the dimension named above; an argument that names none is the same for every part. Nothing has to cross between parts.
All inputs are finite; a program needn't handle non-finite values.
Results may differ from the reference program's by a relative error of at most 0.029.
Values may be sent and summed in bfloat16 or wider, within the bound.
No kernel may reach another device: no remote copies, remote signals or barrier semaphores. Data moves between devices by JAX's collectives and lax.ppermute only.
A program may use at most 192 MiB of HBM per device.

```python
import jax
import jax.numpy as jnp
from jax import lax

D = 2048
FF = 5632
LENGTH = 1024
PROMPTS = 4
N_FS = 4


def block_levels(rng, shape, pieces, least, largest):
    factor_of = 1.0
    for axis_at, blocks in pieces:
        heights = jax.random.uniform(jax.random.fold_in(jax.random.fold_in(rng, 6), axis_at), (blocks,), jnp.float32, least / len(pieces), largest / len(pieces))
        factor_of = factor_of * jnp.repeat(jnp.exp(heights), shape[axis_at] // blocks).reshape((-1,) + (1,) * (len(shape) - 1 - axis_at))
    return factor_of


def bell_draw(key, extent, scale, bound, shards=(), kind=jnp.bfloat16):
    loudness = block_levels(key, extent, shards, -0.22, 0.18) if shards else 1.0
    entries = jax.random.normal(key, extent, jnp.float32) * scale * loudness
    return jnp.minimum(jnp.maximum(entries, -bound), bound).astype(kind)


def setup_inputs(seed: int = 0, part: int = 0) -> dict:
    seeds = jax.random.split(jax.random.key(seed), 9)
    part_keys = jax.random.split(jax.random.fold_in(seeds[8], part), 9)
    prompt = bell_draw(part_keys[0], (PROMPTS, LENGTH, D), 1.0, 6.0, ((0, 4),))
    gate_first = bell_draw(seeds[1], (D, FF), D ** -0.5, 0.125, ((0, 4), (1, 4)), jnp.float32)
    up_first = bell_draw(seeds[2], (D, FF), D ** -0.5, 0.125, ((0, 4), (1, 4)), jnp.float32)
    down_first = bell_draw(seeds[3], (FF, D), (4.0 * FF ** -0.5), 0.3125, ((0, 4), (1, 4)), jnp.float32)
    norm_gain = jnp.clip(1.0 + 0.18 * jax.random.normal(seeds[4], (D,), jnp.float32), 0.1, 1.9)
    gate_second = bell_draw(seeds[5], (D, FF), D ** -0.5, 0.125, ((0, 4), (1, 4)), jnp.float32)
    up_second = bell_draw(seeds[6], (D, FF), D ** -0.5, 0.125, ((0, 4), (1, 4)), jnp.float32)
    down_second = bell_draw(seeds[7], (FF, D), (4.0 * FF ** -0.5), 0.3125, ((0, 4), (1, 4)), jnp.float32)
    return dict(prompt=prompt, gate_first=gate_first, up_first=up_first, down_first=down_first, norm_gain=norm_gain, gate_second=gate_second, up_second=up_second, down_second=down_second)


norm_eps = 1e-05
deep_alpha = 2.0 ** 0.25
half_step = 0.5

def plain_norm(values):
    row_mean = lax.optimization_barrier(jnp.mean(values, axis=-1, keepdims=True))
    centred = values - row_mean
    variance = lax.optimization_barrier(jnp.mean(centred * centred, axis=-1, keepdims=True))
    return centred * lax.rsqrt(variance + norm_eps)

def gated_hidden(inputs, gate_proj, up_proj):
    gate_act = jnp.dot(inputs, gate_proj, preferred_element_type=jnp.float32)
    up_act = jnp.dot(inputs, up_proj, preferred_element_type=jnp.float32)
    return (jax.nn.silu(gate_act) * up_act).astype(jnp.bfloat16)

def block_sums(hidden, down_proj):
    block_width = hidden.shape[1] // N_FS

    def one_block(carried, block_index):
        hidden_block = lax.dynamic_slice_in_dim(hidden, block_index * block_width, block_width, 1)
        down_block = lax.dynamic_slice_in_dim(down_proj, block_index * block_width, block_width, 0)
        partial_term = jnp.dot(hidden_block, down_block, preferred_element_type=jnp.float32).astype(jnp.bfloat16)
        partial_term = lax.optimization_barrier(partial_term)
        return (carried + partial_term.astype(jnp.float32), None)
    start_sum = jnp.zeros((hidden.shape[0], down_proj.shape[1]), jnp.float32)
    summed, unused = lax.scan(one_block, start_sum, jnp.arange(N_FS, dtype=jnp.int32))
    return summed

def reference(prompt, gate_first, up_first, down_first, norm_gain, gate_second, up_second, down_second):
    gate_one = gate_first.astype(jnp.bfloat16)
    up_one = up_first.astype(jnp.bfloat16)
    down_one = down_first.astype(jnp.bfloat16)
    gate_two = (norm_gain[:, None] * gate_second).astype(jnp.bfloat16)
    up_two = (norm_gain[:, None] * up_second).astype(jnp.bfloat16)
    down_two = down_second.astype(jnp.bfloat16)
    tokens = prompt.reshape(-1, prompt.shape[-1])
    hidden_one = gated_hidden(tokens, gate_one, up_one)
    ffn_one = block_sums(hidden_one, down_one)
    normed_one = plain_norm(deep_alpha * tokens.astype(jnp.float32) + half_step * ffn_one).astype(jnp.bfloat16)
    hidden_two = gated_hidden(normed_one, gate_two, up_two)
    ffn_two = block_sums(hidden_two, down_two)
    residual_two = deep_alpha * norm_gain * normed_one.astype(jnp.float32)
    result = plain_norm(residual_two + half_step * ffn_two).astype(jnp.bfloat16).reshape(prompt.shape)
    return (result, gate_one, up_one, down_one, gate_two, up_two, down_two)
```

```python
import jax
import jax.numpy as jnp
from jax import lax
from jax.experimental import pallas as pl
from jax.experimental.pallas import tpu as pltpu
from jax.sharding import PartitionSpec as P

norm_eps = 1e-05
deep_alpha = 2.0**0.25
half_step = 0.5
every_axis = ("grp", "fs", "tp")


def plain_norm(values):
    row_mean = jnp.mean(values, axis=-1, keepdims=True)
    centred = values - row_mean
    variance = jnp.mean(centred * centred, axis=-1, keepdims=True)
    return centred * lax.rsqrt(variance + norm_eps)


def gated_hidden(inputs, gate_proj, up_proj):
    gate_act = jnp.dot(inputs, gate_proj, preferred_element_type=jnp.float32)
    up_act = jnp.dot(inputs, up_proj, preferred_element_type=jnp.float32)
    return (jax.nn.silu(gate_act) * up_act).astype(jnp.bfloat16)


def relay_plain(proj):
    rows = lax.all_gather(proj, "tp", axis=1, tiled=True)
    return lax.all_to_all(rows, "fs", split_axis=1, concat_axis=0, tiled=True)


def paired_mesh(sizes):
    return [sizes[name] for name in every_axis] == [2, 4, 4]


def move(value, target):
    groups, depth, width = (lax.axis_size(name) for name in every_axis)
    pairs = []
    for y in range(groups):
        for z in range(depth):
            for t in range(width):
                y2, z2, x2, c2 = target(y, z, t // 2, t % 2)
                pairs.append(((y * depth + z) * width + t, (y2 * depth + z2) * width + 2 * x2 + c2))
    return lax.ppermute(value, every_axis, pairs)


def swap_chip(value):
    return move(value, lambda y, z, x, c: (y, z, 1 - x, c))


def swap_group(value):
    return move(value, lambda y, z, x, c: (1 - y, z, x, c))


def swap_core(value):
    return move(value, lambda y, z, x, c: (y, z, x, 1 - c))


def plane_of(z, c, hop, depth):
    near = (z - hop) % depth
    return (near, 1 - c) if near % 2 == c else ((near - 1) % depth, c)


def planes_landed(z, c, hop, depth):
    step = (z + c + 1) % 2
    return (z + hop + step) % depth, (z + hop + 1 - step) % depth


def stack_landed(pieces, hops):
    rows, columns = pieces[0].shape

    def kernel(*refs):
        landed = refs[: len(pieces)]
        whole, held, arrived, left = refs[len(pieces) :]
        y, z, t = (lax.axis_index(name) for name in every_axis)
        depth, c = lax.axis_size("fs"), t % 2
        slots = []
        for hop in hops:
            for plane in planes_landed(z, c, hop, depth):
                slots += [plane * 2 + y, plane * 2 + 1 - y]
        loads = [
            pltpu.make_async_copy(piece, held.at[k], arrived.at[k])
            for k, piece in enumerate(landed)
        ]
        stores = [
            pltpu.make_async_copy(held.at[k], whole.at[slot], left.at[k])
            for k, slot in enumerate(slots)
        ]
        for load in loads:
            load.start()
        for load, store in zip(loads, stores):
            load.wait()
            store.start()
        for store in stores:
            store.wait()

    stacked = pl.pallas_call(
        kernel,
        out_shape=jax.ShapeDtypeStruct((len(pieces), rows, columns), pieces[0].dtype),
        in_specs=[pl.BlockSpec(memory_space=pl.ANY)] * len(pieces),
        out_specs=pl.BlockSpec(memory_space=pl.ANY),
        scratch_shapes=[
            pltpu.VMEM((len(pieces), rows, columns), pieces[0].dtype),
            pltpu.SemaphoreType.DMA((len(pieces),)),
            pltpu.SemaphoreType.DMA((len(pieces),)),
        ],
        name="stack_landed",
    )(*pieces)
    return stacked.reshape(len(pieces) * rows, columns)


def relay_paired(proj):
    depth = lax.axis_size("fs")
    y, z, t = (lax.axis_index(name) for name in every_axis)
    x, c = t // 2, t % 2
    rows = proj.shape[0] // 2
    own = lax.dynamic_slice_in_dim(proj, y * rows, rows, 0)
    other = swap_chip(own)
    hops = tuple(reversed(range(0, depth, 2)))
    pieces = []
    for hop in hops:
        near = (z - hop) % depth
        goes = jnp.where(near % 2 == c, near, (near - 1) % depth)
        piece = jnp.where(goes // 2 == x, own, other)

        def target(y, z, x, c, hop=hop):
            plane, core = plane_of(z, c, hop, depth)
            return (y, plane, x, core)

        mine = move(piece, target)
        theirs = swap_group(mine)
        mine_far = swap_core(mine)
        theirs_far = swap_core(theirs)
        pieces += [mine, theirs, mine_far, theirs_far]
    return stack_landed(pieces, hops)


def join_columns(pieces):
    rows, columns = pieces[0].shape

    def kernel(*refs):
        landed = refs[: len(pieces)]
        whole, held, arrived, left = refs[len(pieces) :]
        t = lax.axis_index("tp")
        x, c = t // 2, t % 2
        places = [2 * x + c, 2 * (1 - x) + c, 2 * x + 1 - c, 2 * (1 - x) + 1 - c]
        loads = [
            pltpu.make_async_copy(piece, held.at[k], arrived.at[k])
            for k, piece in enumerate(landed)
        ]
        stores = [
            pltpu.make_async_copy(
                held.at[k], whole.at[:, pl.ds(pl.multiple_of(place * columns, columns), columns)], left.at[k]
            )
            for k, place in enumerate(places)
        ]
        for load in loads:
            load.start()
        for load, store in zip(loads, stores):
            load.wait()
            store.start()
        for store in stores:
            store.wait()

    return pl.pallas_call(
        kernel,
        out_shape=jax.ShapeDtypeStruct((rows, len(pieces) * columns), pieces[0].dtype),
        in_specs=[pl.BlockSpec(memory_space=pl.ANY)] * len(pieces),
        out_specs=pl.BlockSpec(memory_space=pl.ANY),
        scratch_shapes=[
            pltpu.VMEM((len(pieces), rows, columns), pieces[0].dtype),
            pltpu.SemaphoreType.DMA((len(pieces),)),
            pltpu.SemaphoreType.DMA((len(pieces),)),
        ],
        name="join_columns",
    )(*pieces)


def columns_paired(proj):
    other = swap_chip(proj)
    beside = swap_core(proj)
    across = swap_core(other)
    return join_columns([proj, other, beside, across])


def columns_plain(proj):
    return lax.all_gather(proj, "tp", axis=1, tiled=True)


def swap_near(value):
    return move(value, lambda y, z, x, c: (y, z ^ 1, x, c))


def swap_far(value):
    return move(value, lambda y, z, x, c: (y, z ^ 2, x, c))


def row_terms(hidden, down_proj):
    return jnp.dot(hidden, down_proj, preferred_element_type=jnp.float32)


def scatter_paired(terms):
    joined = swap_near(terms[3])
    joined = joined.astype(jnp.float32) + terms[2].astype(jnp.float32)
    far = swap_far(joined.astype(jnp.bfloat16))
    near = swap_near(terms[1])
    return terms[0].astype(jnp.float32) + near.astype(jnp.float32) + far.astype(jnp.float32)


def gather_paired(block):
    far = swap_far(block)
    near = swap_near(block)
    last = swap_near(far)
    return jnp.concatenate([block, near, far, last], axis=0)


def paired_ffn(tokens, norm_gain, one, two):
    gate_one, up_one, down_one = one
    gate_two, up_two, down_two = two
    planes, parts = 4, 2
    z = lax.axis_index("fs")
    own_count = tokens.shape[0] // planes
    rows = own_count // parts

    def terms_of(inputs, gate_proj, up_proj, down_proj):
        hidden = gated_hidden(inputs, gate_proj, up_proj)
        terms = row_terms(hidden, down_proj).astype(jnp.bfloat16)
        return [terms[k * rows : (k + 1) * rows] for k in range(planes)]

    owned, sent = [], []
    for part in range(parts):
        blocks = [lax.dynamic_slice_in_dim(tokens, (z ^ k) * own_count + part * rows, rows, 0) for k in range(planes)]
        owned.append(blocks[0])
        sent.append(terms_of(jnp.concatenate(blocks, axis=0), gate_one, up_one, down_one))
    normed, again = [], []
    for part in range(parts):
        ffn_one = scatter_paired(sent[part])
        normed.append(
            plain_norm(
                deep_alpha * owned[part].astype(jnp.float32) + half_step * ffn_one
            ).astype(jnp.bfloat16)
        )
        inputs = gather_paired(normed[part])
        again.append(terms_of(inputs, gate_two, up_two, down_two))
    results = []
    for part in range(parts):
        ffn_two = scatter_paired(again[part])
        residual_two = deep_alpha * norm_gain * normed[part].astype(jnp.float32)
        results.append(plain_norm(residual_two + half_step * ffn_two).astype(jnp.bfloat16))
    return jnp.concatenate(results, axis=0)


def plain_ffn(tokens, norm_gain, one, two):
    gate_one, up_one, down_one = one
    gate_two, up_two, down_two = two
    own_count = tokens.shape[0] // lax.axis_size("fs")
    own_first = lax.axis_index("fs") * own_count
    hidden_one = gated_hidden(tokens, gate_one, up_one)
    own_tokens = lax.dynamic_slice_in_dim(tokens, own_first, own_count, 0)
    ffn_one = lax.psum_scatter(
        row_terms(hidden_one, down_one).astype(jnp.bfloat16), "fs", scatter_dimension=0, tiled=True
    ).astype(jnp.float32)
    normed_own = plain_norm(
        deep_alpha * own_tokens.astype(jnp.float32) + half_step * ffn_one
    ).astype(jnp.bfloat16)
    hidden_two = gated_hidden(
        lax.all_gather(normed_own, "fs", axis=0, tiled=True), gate_two, up_two
    )
    ffn_two = lax.psum_scatter(
        row_terms(hidden_two, down_two).astype(jnp.bfloat16), "fs", scatter_dimension=0, tiled=True
    ).astype(jnp.float32)
    residual_two = deep_alpha * norm_gain * normed_own.astype(jnp.float32)
    return plain_norm(residual_two + half_step * ffn_two).astype(jnp.bfloat16)


def body(prompt, gate_first, up_first, down_first, norm_gain, gate_second, up_second, down_second):
    paired = paired_mesh({name: lax.axis_size(name) for name in every_axis})
    relay = relay_paired if paired else relay_plain
    columns = columns_paired if paired else columns_plain
    fs_index = lax.axis_index("fs")
    row_block = gate_first.shape[0]
    gain_rows = lax.dynamic_slice_in_dim(norm_gain, fs_index * row_block, row_block, 0)
    up_one = relay(up_first.astype(jnp.bfloat16))
    gate_one = relay(gate_first.astype(jnp.bfloat16))
    down_one = columns(down_first.astype(jnp.bfloat16))
    up_two = relay((gain_rows[:, None] * up_second).astype(jnp.bfloat16))
    gate_two = relay((gain_rows[:, None] * gate_second).astype(jnp.bfloat16))
    down_two = columns(down_second.astype(jnp.bfloat16))
    tokens = prompt.reshape(-1, prompt.shape[-1])
    one, two = (gate_one, up_one, down_one), (gate_two, up_two, down_two)
    result = (paired_ffn if paired else plain_ffn)(tokens, norm_gain, one, two)
    return (
        result.reshape(1, result.shape[0], result.shape[-1]),
        gate_one,
        up_one,
        down_one,
        gate_two,
        up_two,
        down_two,
    )


def solution(mesh):
    placed = (
        P(("grp", "tp"), None, None),
        P("fs", "tp"),
        P("fs", "tp"),
        P("fs", "tp"),
        P(),
        P("fs", "tp"),
        P("fs", "tp"),
        P("fs", "tp"),
    )
    return jax.shard_map(
        body,
        mesh=mesh,
        in_specs=placed,
        out_specs=(
            P(("grp", "tp"), "fs", None),
            P("grp", "fs"),
            P("grp", "fs"),
            P("fs", "grp"),
            P("grp", "fs"),
            P("grp", "fs"),
            P("fs", "grp"),
        ),
        check_vma=False,
    )
```

```python
import jax
import jax.numpy as jnp
from jax import lax
from jax.experimental import pallas as pl
from jax.experimental.pallas import tpu as pltpu
from jax.sharding import PartitionSpec as P

norm_eps = 1e-05
deep_alpha = 2.0**0.25
half_step = 0.5
every_axis = ("grp", "fs", "tp")


def plain_norm(values):
    row_mean = jnp.mean(values, axis=-1, keepdims=True)
    centred = values - row_mean
    variance = jnp.mean(centred * centred, axis=-1, keepdims=True)
    return centred * lax.rsqrt(variance + norm_eps)


def gated_hidden(inputs, gate_proj, up_proj):
    gate_act = jnp.dot(inputs, gate_proj, preferred_element_type=jnp.float32)
    up_act = jnp.dot(inputs, up_proj, preferred_element_type=jnp.float32)
    return (jax.nn.silu(gate_act) * up_act).astype(jnp.bfloat16)


def relay_plain(*projs):
    rows = [lax.all_gather(proj, "tp", axis=1, tiled=True) for proj in projs]
    return [lax.all_to_all(part, "fs", split_axis=1, concat_axis=0, tiled=True) for part in rows]


def paired_mesh(sizes):
    return [sizes[name] for name in every_axis] == [2, 4, 4]


def move(value, target):
    groups, depth, width = (lax.axis_size(name) for name in every_axis)
    pairs = []
    for y in range(groups):
        for z in range(depth):
            for t in range(width):
                y2, z2, x2, c2 = target(y, z, t // 2, t % 2)
                pairs.append(((y * depth + z) * width + t, (y2 * depth + z2) * width + 2 * x2 + c2))
    return lax.ppermute(value, every_axis, pairs)


def swap_chip(value):
    return move(value, lambda y, z, x, c: (y, z, 1 - x, c))


def swap_group(value):
    return move(value, lambda y, z, x, c: (1 - y, z, x, c))


def swap_core(value):
    return move(value, lambda y, z, x, c: (y, z, x, 1 - c))


def plane_of(z, c, hop, depth):
    near = (z - hop) % depth
    return (near, 1 - c) if near % 2 == c else ((near - 1) % depth, c)


def planes_landed(z, c, hop, depth):
    step = (z + c + 1) % 2
    return (z + hop + step) % depth, (z + hop + 1 - step) % depth


def stack_landed(pieces, hops):
    count, rows, columns = pieces[0].shape

    def kernel(*refs):
        landed, wholes = refs[: len(pieces)], refs[len(pieces) : len(pieces) + count]
        held, arrived, left = refs[len(pieces) + count :]
        y, z, t = (lax.axis_index(name) for name in every_axis)
        depth, c = lax.axis_size("fs"), t % 2
        slots = []
        for hop in hops:
            for plane in planes_landed(z, c, hop, depth):
                slots += [plane * 2 + y, plane * 2 + 1 - y]
        loads = [
            pltpu.make_async_copy(piece, held.at[k], arrived.at[k])
            for k, piece in enumerate(landed)
        ]
        stores = [
            [
                pltpu.make_async_copy(held.at[k, i], whole.at[slot], left.at[i, k])
                for i, whole in enumerate(wholes)
            ]
            for k, slot in enumerate(slots)
        ]
        for load in loads:
            load.start()
        for load, outs in zip(loads, stores):
            load.wait()
            for out in outs:
                out.start()
        for outs in stores:
            for out in outs:
                out.wait()

    stacked = pl.pallas_call(
        kernel,
        out_shape=[jax.ShapeDtypeStruct((len(pieces), rows, columns), pieces[0].dtype)] * count,
        in_specs=[pl.BlockSpec(memory_space=pl.ANY)] * len(pieces),
        out_specs=[pl.BlockSpec(memory_space=pl.ANY)] * count,
        scratch_shapes=[
            pltpu.VMEM((len(pieces), count, rows, columns), pieces[0].dtype),
            pltpu.SemaphoreType.DMA((len(pieces),)),
            pltpu.SemaphoreType.DMA((count, len(pieces))),
        ],
        name="stack_landed",
    )(*pieces)
    return [whole.reshape(len(pieces) * rows, columns) for whole in stacked]


def relay_paired(*projs):
    depth = lax.axis_size("fs")
    y, z, t = (lax.axis_index(name) for name in every_axis)
    x, c = t // 2, t % 2
    rows = projs[0].shape[0] // 2
    own = jnp.stack([lax.dynamic_slice_in_dim(proj, y * rows, rows, 0) for proj in projs])
    other = swap_chip(own)
    hops = tuple(reversed(range(0, depth, 2)))
    pieces = []
    for hop in hops:
        near = (z - hop) % depth
        goes = jnp.where(near % 2 == c, near, (near - 1) % depth)
        piece = jnp.where(goes // 2 == x, own, other)

        def target(y, z, x, c, hop=hop):
            plane, core = plane_of(z, c, hop, depth)
            return (y, plane, x, core)

        mine = move(piece, target)
        theirs = swap_group(mine)
        mine_far = swap_core(mine)
        theirs_far = swap_core(theirs)
        pieces += [mine, theirs, mine_far, theirs_far]
    return stack_landed(pieces, hops)


def join_columns(pieces):
    rows, columns = pieces[0].shape

    def kernel(*refs):
        landed = refs[: len(pieces)]
        whole, held, arrived, left = refs[len(pieces) :]
        t = lax.axis_index("tp")
        x, c = t // 2, t % 2
        places = [2 * x + c, 2 * (1 - x) + c, 2 * x + 1 - c, 2 * (1 - x) + 1 - c]
        loads = [
            pltpu.make_async_copy(piece, held.at[k], arrived.at[k])
            for k, piece in enumerate(landed)
        ]
        stores = [
            pltpu.make_async_copy(
                held.at[k], whole.at[:, pl.ds(pl.multiple_of(place * columns, columns), columns)], left.at[k]
            )
            for k, place in enumerate(places)
        ]
        for load in loads:
            load.start()
        for load, store in zip(loads, stores):
            load.wait()
            store.start()
        for store in stores:
            store.wait()

    return pl.pallas_call(
        kernel,
        out_shape=jax.ShapeDtypeStruct((rows, len(pieces) * columns), pieces[0].dtype),
        in_specs=[pl.BlockSpec(memory_space=pl.ANY)] * len(pieces),
        out_specs=pl.BlockSpec(memory_space=pl.ANY),
        scratch_shapes=[
            pltpu.VMEM((len(pieces), rows, columns), pieces[0].dtype),
            pltpu.SemaphoreType.DMA((len(pieces),)),
            pltpu.SemaphoreType.DMA((len(pieces),)),
        ],
        name="join_columns",
    )(*pieces)


def columns_paired(proj):
    other = swap_chip(proj)
    beside = swap_core(proj)
    across = swap_core(other)
    return join_columns([proj, other, beside, across])


def columns_plain(proj):
    return lax.all_gather(proj, "tp", axis=1, tiled=True)


def swap_near(value):
    return move(value, lambda y, z, x, c: (y, z ^ 1, x, c))


def swap_far(value):
    return move(value, lambda y, z, x, c: (y, z ^ 2, x, c))


def row_terms(hidden, down_proj):
    return jnp.dot(hidden, down_proj, preferred_element_type=jnp.float32)


def scatter_paired(terms):
    joined = swap_near(terms[3])
    joined = joined.astype(jnp.float32) + terms[2].astype(jnp.float32)
    far = swap_far(joined.astype(jnp.bfloat16))
    near = swap_near(terms[1])
    return terms[0].astype(jnp.float32) + near.astype(jnp.float32) + far.astype(jnp.float32)


def gather_paired(block):
    far = swap_far(block)
    near = swap_near(block)
    last = swap_near(far)
    return jnp.concatenate([block, near, far, last], axis=0)


def paired_ffn(tokens, norm_gain, one, two):
    gate_one, up_one, down_one = one
    gate_two, up_two, down_two = two
    planes, z = 4, lax.axis_index("fs")
    own_count = tokens.shape[0] // planes
    later = own_count // 2
    spans = ((0, own_count - later), (own_count - later, later))

    def terms_of(inputs, gate_proj, up_proj, down_proj):
        rows = inputs.shape[0] // planes
        hidden = gated_hidden(inputs, gate_proj, up_proj)
        terms = row_terms(lax.optimization_barrier(hidden), down_proj).astype(jnp.bfloat16)
        return [terms[k * rows : (k + 1) * rows] for k in range(planes)]

    owned, sent = [], []
    for start, rows in spans:
        blocks = [
            lax.dynamic_slice_in_dim(tokens, (z ^ k) * own_count + start, rows, 0)
            for k in range(planes)
        ]
        owned.append(blocks[0])
        sent.append(terms_of(jnp.concatenate(blocks, axis=0), gate_one, up_one, down_one))
    normed, again = [], []
    for part in range(len(spans)):
        ffn_one = scatter_paired(sent[part])
        normed.append(
            plain_norm(
                deep_alpha * owned[part].astype(jnp.float32) + half_step * ffn_one
            ).astype(jnp.bfloat16)
        )
        inputs = gather_paired(normed[part])
        again.append(terms_of(inputs, gate_two, up_two, down_two))
    results = []
    for part in range(len(spans)):
        ffn_two = scatter_paired(again[part])
        residual_two = deep_alpha * norm_gain * normed[part].astype(jnp.float32)
        results.append(plain_norm(residual_two + half_step * ffn_two).astype(jnp.bfloat16))
    return jnp.concatenate(results, axis=0)


def plain_ffn(tokens, norm_gain, one, two):
    gate_one, up_one, down_one = one
    gate_two, up_two, down_two = two
    own_count = tokens.shape[0] // lax.axis_size("fs")
    own_first = lax.axis_index("fs") * own_count
    hidden_one = gated_hidden(tokens, gate_one, up_one)
    own_tokens = lax.dynamic_slice_in_dim(tokens, own_first, own_count, 0)
    ffn_one = lax.psum_scatter(
        row_terms(hidden_one, down_one).astype(jnp.bfloat16), "fs", scatter_dimension=0, tiled=True
    ).astype(jnp.float32)
    normed_own = plain_norm(
        deep_alpha * own_tokens.astype(jnp.float32) + half_step * ffn_one
    ).astype(jnp.bfloat16)
    hidden_two = gated_hidden(
        lax.all_gather(normed_own, "fs", axis=0, tiled=True), gate_two, up_two
    )
    ffn_two = lax.psum_scatter(
        row_terms(hidden_two, down_two).astype(jnp.bfloat16), "fs", scatter_dimension=0, tiled=True
    ).astype(jnp.float32)
    residual_two = deep_alpha * norm_gain * normed_own.astype(jnp.float32)
    return plain_norm(residual_two + half_step * ffn_two).astype(jnp.bfloat16)


def body(prompt, gate_first, up_first, down_first, norm_gain, gate_second, up_second, down_second):
    paired = paired_mesh({name: lax.axis_size(name) for name in every_axis})
    relay = relay_paired if paired else relay_plain
    columns = columns_paired if paired else columns_plain
    fs_index = lax.axis_index("fs")
    row_block = gate_first.shape[0]
    gain_rows = lax.dynamic_slice_in_dim(norm_gain, fs_index * row_block, row_block, 0)
    (gate_one,) = relay(gate_first.astype(jnp.bfloat16))
    (up_one,) = relay(up_first.astype(jnp.bfloat16))
    down_one = columns(down_first.astype(jnp.bfloat16))
    up_two, gate_two = relay(
        (gain_rows[:, None] * up_second).astype(jnp.bfloat16),
        (gain_rows[:, None] * gate_second).astype(jnp.bfloat16),
    )
    down_two = columns(down_second.astype(jnp.bfloat16))
    tokens = prompt.reshape(-1, prompt.shape[-1])
    one, two = (gate_one, up_one, down_one), (gate_two, up_two, down_two)
    result = (paired_ffn if paired else plain_ffn)(tokens, norm_gain, one, two)
    return (
        result.reshape(1, result.shape[0], result.shape[-1]),
        gate_one,
        up_one,
        down_one,
        gate_two,
        up_two,
        down_two,
    )


def solution(mesh):
    placed = (
        P(("grp", "tp"), None, None),
        P("fs", "tp"),
        P("fs", "tp"),
        P("fs", "tp"),
        P(),
        P("fs", "tp"),
        P("fs", "tp"),
        P("fs", "tp"),
    )
    return jax.shard_map(
        body,
        mesh=mesh,
        in_specs=placed,
        out_specs=(
            P(("grp", "tp"), "fs", None),
            P("grp", "fs"),
            P("grp", "fs"),
            P("fs", "grp"),
            P("grp", "fs"),
            P("grp", "fs"),
            P("fs", "grp"),
        ),
        check_vma=False,
    )
```
